32 devices in a mesh: kv: 8 (over z, y), tp: 4 (over x, core).
Axes of the slice: x: 2, y: 2, z: 4, core: 2. Of those that a mesh axis runs over, the one named last changes fastest.
Arguments:
- tokens: bfloat16 [128, 4096], P(None, ('kv', 'tp')), may hold values from -64 to 64
- mix_gain: float32 [4096], P('kv'), may hold values from 0.1 to 1.9
- w_query: bfloat16 [4096, 3072], P('kv', 'tp'), may hold values from -0.09375 to 0.09375
- w_key: bfloat16 [4096, 3072], P('kv', 'tp'), may hold values from -0.09375 to 0.09375
- w_value: bfloat16 [4096, 3072], P('kv', 'tp'), may hold values from -0.09375 to 0.09375
- w_gate: bfloat16 [4096, 3072], P('kv', 'tp'), may hold values from -0.09375 to 0.09375
- w_beta: bfloat16 [4096, 24], P('kv'), may hold values from -0.09375 to 0.09375
- w_decay: bfloat16 [4096, 24], P('kv'), may hold values from -0.09375 to 0.09375
- decay_rate: float32 [24], P('tp'), may hold values from 0.15 to 1.5
- out_gain: float32 [128], replicated, may hold values from 0.1 to 1.9
- state: float32 [128, 24, 128, 128], P('kv', 'tp'), may hold values from -0.6 to 0.6
- w_out: bfloat16 [3072, 4096], P('tp', 'kv'), may hold values from -0.109375 to 0.109375
- mlp_gain: float32 [4096], replicated, may hold values from 0.1 to 1.9
- w_up: bfloat16 [4096, 16384], P(None, ('kv', 'tp')), may hold values from -0.09375 to 0.09375
- w_down: bfloat16 [16384, 4096], P(('kv', 'tp')), may hold values from -0.09375 to 0.09375
Outputs:
- mixed: bfloat16 [128, 4096], P(None, ('kv', 'tp'))
- new_state: float32 [128, 24, 128, 128], P('kv', 'tp')
The draws below stay inside these ranges and needn't reach their ends.
All inputs are finite; a program needn't handle non-finite values.
Results may differ from the reference program's by a relative error of at most 0.0063.
Values may be sent and summed in bfloat16 or wider, within the bound.
A program may use at most 64 MiB of HBM per device.

```python
import math
import jax
import jax.numpy as jnp
from jax import lax

D = 4096
H = 24
HEAD = 128
FF = 16384
BATCH = 128


def draw_tokens(key, part):
    first, second, third = jax.random.split(jax.random.fold_in(key, 17), 3)
    position = jnp.arange(D, dtype=jnp.float32) / D
    column_scale = jnp.exp(jnp.log(6.0) * (position - 0.5)) * jax.random.uniform(second, (D,), jnp.float32, 0.6, 1.6)
    base = jnp.clip(jax.random.normal(first, (BATCH, D), jnp.float32), -4.0, 4.0)
    row_scale = jnp.exp(jax.random.uniform(third, (BATCH, 1), jnp.float32, jnp.log(0.4), jnp.log(4.0)))
    values = base * row_scale * column_scale[None, :]
    return values.astype(jnp.bfloat16)


def raised(entries, rng, source, target, parts, factor):
    owner, partner = [(jnp.arange(entries.shape[dim]) // (entries.shape[dim] // parts)).reshape([-1 if axis == dim else 1 for axis in range(entries.ndim)]) for dim in (source, target)]
    chosen = jax.random.permutation(rng, parts)[partner]
    strong = (owner == chosen) | (owner == (partner + parts // 2) % parts)
    return jnp.where(strong, factor * entries, entries)


def levels(own_key, extent, cuts, least, top_value):
    def one(dim, parts):
        steps = jax.random.uniform(jax.random.fold_in(jax.random.fold_in(own_key, 6), dim), (parts,), jnp.float32, least / len(cuts), top_value / len(cuts))
        return jnp.repeat(jnp.exp(steps), extent[dim] // parts).reshape((-1,) + (1,) * (len(extent) - dim - 1))

    level = one(*cuts[0])
    for cut in cuts[1:]:
        level = level * one(*cut)
    return level


def noise(own_key, extent, deviation, bound, cuts=(), kind=jnp.bfloat16):
    values = deviation * jax.random.normal(own_key, extent, jnp.float32)
    if cuts:
        values = values * levels(own_key, extent, cuts, -0.22, 0.18)
    return jnp.clip(values, -bound, bound).astype(kind)


def gaussian_with(rng, dims, deviation, limit, pieces, heavy, kind=jnp.bfloat16):
    values = deviation * jax.random.normal(rng, dims, jnp.float32)
    if pieces:
        values = values * levels(rng, dims, pieces, -0.22, 0.18)
    return jnp.clip(raised(values, jax.random.fold_in(rng, 3), *heavy), -limit, limit).astype(kind)


def setup_inputs(seed: int = 0) -> dict:
    key_of = jax.random.split(jax.random.key(seed), 16)
    return {
        "tokens": draw_tokens(jax.random.fold_in(key_of[15], 71), 0),
        "mix_gain": jnp.clip(1.0 + 0.18 * jax.random.normal(key_of[1], (D,), jnp.float32), 0.1, 1.9),
        "w_query": noise(key_of[2], (D, H * HEAD), D ** -0.5, 0.09375, ((0, 8), (1, 4))),
        "w_key": noise(key_of[3], (D, H * HEAD), D ** -0.5, 0.09375, ((0, 8), (1, 4))),
        "w_value": noise(key_of[4], (D, H * HEAD), D ** -0.5, 0.09375, ((0, 8), (1, 4))),
        "w_gate": noise(key_of[5], (D, H * HEAD), D ** -0.5, 0.09375, ((0, 8), (1, 4))),
        "w_beta": noise(key_of[6], (D, H), D ** -0.5, 0.09375, ((0, 8),)),
        "w_decay": noise(key_of[7], (D, H), D ** -0.5, 0.09375, ((0, 8),)),
        "decay_rate": jnp.clip(jnp.exp(math.log(1.5) - 2.3025851 * jax.random.uniform(key_of[8], (H,), jnp.float32) ** levels(key_of[8], (H,), ((0, 4),), -0.2, 0.2)), 0.15, 1.5),
        "out_gain": jnp.clip(1.0 + 0.18 * jax.random.normal(key_of[9], (HEAD,), jnp.float32), 0.1, 1.9),
        "state": noise(key_of[10], (BATCH, H, HEAD, HEAD), 0.1, 0.6, ((0, 8), (1, 4)), jnp.float32),
        "w_out": noise(key_of[11], (H * HEAD, D), (H * HEAD) ** -0.5, 0.109375, ((0, 4), (1, 8))),
        "mlp_gain": jnp.clip(1.0 + 0.18 * jax.random.normal(key_of[12], (D,), jnp.float32), 0.1, 1.9),
        "w_up": noise(key_of[13], (D, FF), D ** -0.5, 0.09375, ((1, 32),)),
        "w_down": gaussian_with(key_of[14], (FF, D), FF ** -0.5, 0.09375, ((0, 32),), (0, 1, 32, 2.75)),
    }


EPSILON = 1e-06

def head_norm(values):
    return values * lax.rsqrt(lax.optimization_barrier(jnp.sum(values * values, axis=-1, keepdims=True)) + EPSILON)

def per_head(inputs):
    old_state, decay, key, value, beta, query = inputs
    faded = old_state * decay[:, None, None]
    recalled = jnp.einsum('bkv,bk->bv', faded, key, precision=lax.Precision.HIGHEST)
    change = beta[:, None] * (value - recalled)
    updated = faded + key[:, :, None] * change[:, None, :]
    readout = jnp.einsum('bkv,bk->bv', updated, query, precision=lax.Precision.HIGHEST)
    return (updated, readout)

def reference(tokens, mix_gain, w_query, w_key, w_value, w_gate, w_beta, w_decay, decay_rate, out_gain, state, w_out, mlp_gain, w_up, w_down):
    tokens_f = tokens.astype(jnp.float32)
    row_scale = lax.rsqrt(lax.optimization_barrier(jnp.mean(tokens_f * tokens_f, axis=1, keepdims=True)) + EPSILON)
    normed = (tokens_f * mix_gain[None, :]).astype(jnp.bfloat16)

    def project(weight):
        return jnp.dot(normed, weight, preferred_element_type=jnp.float32) * row_scale
    query_raw = project(w_query).reshape(BATCH, H, HEAD)
    key_raw = project(w_key).reshape(BATCH, H, HEAD)
    value_raw = project(w_value).reshape(BATCH, H, HEAD)
    gate_raw = project(w_gate).reshape(BATCH, H, HEAD)
    beta_raw = project(w_beta)
    decay_raw = project(w_decay)
    query = head_norm(jax.nn.silu(query_raw)) * HEAD ** (-0.5)
    key = head_norm(jax.nn.silu(key_raw))
    value = jax.nn.silu(value_raw)
    beta = jax.nn.sigmoid(beta_raw)
    decay = jnp.exp(-decay_rate[None, :] * jax.nn.softplus(decay_raw))
    updated, readout = lax.map(per_head, (jnp.moveaxis(state, 1, 0), decay.T, jnp.moveaxis(key, 1, 0), jnp.moveaxis(value, 1, 0), beta.T, jnp.moveaxis(query, 1, 0)))
    new_state = jnp.moveaxis(updated, 0, 1)
    readout = jnp.moveaxis(readout, 0, 1)
    scaled = readout * lax.rsqrt(lax.optimization_barrier(jnp.mean(readout * readout, axis=-1, keepdims=True)) + EPSILON) * out_gain
    merged = (scaled * jax.nn.silu(gate_raw)).reshape(BATCH, H * HEAD).astype(jnp.bfloat16)
    residual = (tokens_f + jnp.dot(merged, w_out, preferred_element_type=jnp.float32)).astype(jnp.bfloat16)
    residual_f = residual.astype(jnp.float32)
    normed_mlp = (residual_f * lax.rsqrt(lax.optimization_barrier(jnp.mean(residual_f * residual_f, axis=1, keepdims=True)) + EPSILON) * mlp_gain[None, :]).astype(jnp.bfloat16)
    hidden = jnp.square(jax.nn.relu(jnp.dot(normed_mlp, w_up, preferred_element_type=jnp.float32))).astype(jnp.bfloat16)
    mixed = (residual_f + jnp.dot(hidden, w_down, preferred_element_type=jnp.float32)).astype(jnp.bfloat16)
    return (mixed, new_state)
```

```python
import functools
import math

import jax
import jax.numpy as jnp
from jax import lax
from jax.experimental import pallas as pl
from jax.experimental.pallas import tpu as pltpu
from jax.sharding import PartitionSpec as P

EPSILON = 1e-06
CORES = 2
VMEM_BYTES = 60 * 2**20
BF16 = jnp.bfloat16
F32 = jnp.float32


class Grid:
    def __init__(self, n_kv, n_tp):
        self.n_kv, self.n_tp = n_kv, n_tp
        low = max(f for f in range(1, math.isqrt(n_kv) + 1) if n_kv % f == 0)
        self.n_lo, self.n_hi = low, n_kv // low
        self.n_core = CORES if n_tp % CORES == 0 else 1
        self.n_x = n_tp // self.n_core
        self.plane = [
            (dy, dx) for dy in range(self.n_lo) for dx in range(self.n_x) if (dy, dx) != (0, 0)
        ]

    def locate(self):
        self.kv, self.tp = lax.axis_index("kv"), lax.axis_index("tp")
        self.hi, self.lo = self.kv // self.n_lo, lax.rem(self.kv, self.n_lo)
        self.x, self.core = self.tp // self.n_core, lax.rem(self.tp, self.n_core)

    def at(self, hi, lo, x, core):
        return (hi * self.n_lo + lo, x * self.n_core + core)


def step(index, offset, size):
    return lax.rem(index + (offset % size), size) if offset % size else index


def send(src, dst, send_sem, recv_sem, device):
    copy = pltpu.make_async_remote_copy(
        src_ref=src,
        dst_ref=dst,
        send_sem=send_sem,
        recv_sem=recv_sem,
        device_id=device,
        device_id_type=pl.DeviceIdType.MESH,
    )
    copy.start()
    return copy


def greet(peers):
    barrier = pltpu.get_barrier_semaphore()
    for peer in peers:
        pl.semaphore_signal(barrier, inc=1, device_id=peer, device_id_type=pl.DeviceIdType.MESH)
    pl.semaphore_wait(barrier, len(peers))


def project_kernel(
    grid, rate_width,
    tok_ref, gain_ref, wq_ref, wk_ref, wv_ref, wg_ref, wr_ref,
    out_ref, rate_ref,
    cols, part, rate_part, near_send, near_recv, far_send, far_recv, rate_recv,
    own_sem, tok_sems, near_sems, far_sems, rate_sems,
):
    g = grid
    g.locate()
    n_kv, n_tp, n_lo, n_hi = g.n_kv, g.n_tp, g.n_lo, g.n_hi
    local = pltpu.make_async_copy(tok_ref, cols.at[g.tp], own_sem)
    local.start()
    greet(
        [(g.kv, step(g.tp, k, n_tp)) for k in range(1, n_tp)]
        + [(step(g.kv, k, n_kv), g.tp) for k in range(1, n_kv)]
    )
    started = [
        send(tok_ref, cols.at[g.tp], tok_sems.at[0, k], tok_sems.at[1, k],
             (g.kv, step(g.tp, k, n_tp)))
        for k in range(1, n_tp)
    ]
    local.wait()
    for copy in started:
        copy.wait()
    size = tok_ref.shape[1]
    rows = part.shape[2]
    blocks = [cols[i].astype(F32) for i in range(n_tp)]
    squares = sum(jnp.sum(b * b, axis=1, keepdims=True) for b in blocks)
    normed = [(blocks[i] * gain_ref[i]).astype(BF16) for i in range(n_tp)]
    if size % 128 == 0:
        normed = [jnp.concatenate(normed, axis=1)]
    depth = normed[0].shape[1]

    def product(w_ref):
        return sum(
            jnp.dot(normed[i], w_ref[i * depth : (i + 1) * depth, :], preferred_element_type=F32)
            for i in range(len(normed))
        )

    rates = product(wr_ref)
    lane = lax.broadcasted_iota(jnp.int32, rates.shape, 1)
    rates = jnp.where(lane == rate_width, squares, rates)
    rate_part[...] = rates.reshape(n_kv, rows, rates.shape[1])
    rate_copies = [
        send(rate_part.at[step(g.kv, k, n_kv)], rate_recv.at[k], rate_sems.at[0, k],
             rate_sems.at[1, k], (step(g.kv, k, n_kv), g.tp))
        for k in range(1, n_kv)
    ]
    near = {}
    for c, w_ref in enumerate((wq_ref, wk_ref, wv_ref, wg_ref)):
        value = product(w_ref).reshape(n_kv, rows, w_ref.shape[1])
        part[c] = value
        for lo in range(n_lo):
            for hi in range(n_hi):
                near_send[c, lo, hi] = value[hi * n_lo + lo].astype(BF16)
        for k in range(1, n_lo):
            lo = step(g.lo, k, n_lo)
            near[c, k] = send(near_send.at[c, lo], near_recv.at[c, k], near_sems.at[0, c, k],
                              near_sems.at[1, c, k], (g.hi * n_lo + lo, g.tp))
    far = {}
    for c in range(4):
        for k in range(1, n_lo):
            near[c, k].wait()
        for d in list(range(1, n_hi)) + [0]:
            hi = step(g.hi, d, n_hi)
            total = part[c, hi * n_lo + g.lo]
            for k in range(1, n_lo):
                total = total + near_recv[c, k, hi].astype(F32)
            if d == 0:
                out_ref[c] = total
            else:
                far_send[c, d] = total.astype(BF16)
                far[c, d] = send(far_send.at[c, d], far_recv.at[c, d], far_sems.at[0, c, d],
                                 far_sems.at[1, c, d], (hi * n_lo + g.lo, g.tp))
    for copy in rate_copies:
        copy.wait()
    rate_total = rate_part[g.kv]
    for k in range(1, n_kv):
        rate_total = rate_total + rate_recv[k]
    rate_ref[...] = rate_total
    for c in range(4):
        total = out_ref[c]
        for d in range(1, n_hi):
            far[c, d].wait()
            total = total + far_recv[c, d].astype(F32)
        out_ref[c] = total


def project(grid, tokens, mix_gain, weights, w_rates, rate_width):
    g = grid
    batch, size = tokens.shape
    rows, width = batch // g.n_kv, weights[0].shape[1]
    lanes = w_rates.shape[1]
    vmem = pl.BlockSpec(memory_space=pltpu.VMEM)
    dma = pltpu.SemaphoreType.DMA
    return pl.pallas_call(
        functools.partial(project_kernel, g, rate_width),
        out_shape=(
            jax.ShapeDtypeStruct((4, rows, width), F32),
            jax.ShapeDtypeStruct((rows, lanes), F32),
        ),
        in_specs=[vmem] * 7,
        out_specs=(vmem, vmem),
        scratch_shapes=[
            pltpu.VMEM((g.n_tp, batch, size), BF16),
            pltpu.VMEM((4, g.n_kv, rows, width), F32),
            pltpu.VMEM((g.n_kv, rows, lanes), F32),
            pltpu.VMEM((4, g.n_lo, g.n_hi, rows, width), BF16),
            pltpu.VMEM((4, g.n_lo, g.n_hi, rows, width), BF16),
            pltpu.VMEM((4, g.n_hi, rows, width), BF16),
            pltpu.VMEM((4, g.n_hi, rows, width), BF16),
            pltpu.VMEM((g.n_kv, rows, lanes), F32),
            dma,
            dma((2, g.n_tp)),
            dma((2, 4, g.n_lo)),
            dma((2, 4, g.n_hi)),
            dma((2, g.n_kv)),
        ],
        compiler_params=pltpu.CompilerParams(
            collective_id=0, has_side_effects=True, vmem_limit_bytes=VMEM_BYTES
        ),
        name="project",
    )(tokens, mix_gain.reshape(g.n_tp, 1, size), *weights, w_rates)


def state_kernel(s_ref, kt_ref, qt_ref, value_ref, gate_ref, decay_ref, beta_ref, gain_ref,
                 new_ref, merged_ref):
    for h in range(s_ref.shape[1]):
        row = slice(h, h + 1)
        faded = s_ref[0, h] * decay_ref[0, row, :]
        key = kt_ref[0, :, row]
        recalled = jnp.sum(faded * key, axis=0, keepdims=True)
        change = beta_ref[0, row, :] * (value_ref[0, row, :] - recalled)
        updated = faded + key * change
        new_ref[0, h] = updated
        readout = jnp.sum(updated * qt_ref[0, :, row], axis=0, keepdims=True)
        scaled = (
            readout
            * lax.rsqrt(jnp.mean(readout * readout, axis=1, keepdims=True) + EPSILON)
            * gain_ref[...]
        )
        merged_ref[0, row, :] = scaled * gate_ref[0, row, :]


def update_state(state, key, query, value, gate, decay, beta, out_gain):
    rows, heads, size, _ = state.shape
    whole = pl.BlockSpec((1, heads, size, size), lambda i: (i, 0, 0, 0))
    tall = pl.BlockSpec((1, size, heads), lambda i: (i, 0, 0))
    wide = pl.BlockSpec((1, heads, size), lambda i: (i, 0, 0))
    return pl.pallas_call(
        state_kernel,
        grid=(rows,),
        out_shape=(
            jax.ShapeDtypeStruct(state.shape, F32),
            jax.ShapeDtypeStruct((rows, heads, size), F32),
        ),
        in_specs=[whole, tall, tall, wide, wide, wide, wide,
                  pl.BlockSpec((1, size), lambda i: (0, 0))],
        out_specs=(whole, wide),
        compiler_params=pltpu.CompilerParams(dimension_semantics=("arbitrary",)),
        name="state",
    )(
        state,
        jnp.swapaxes(key, 1, 2),
        jnp.swapaxes(query, 1, 2),
        value,
        gate,
        jnp.broadcast_to(decay[:, :, None], value.shape),
        jnp.broadcast_to(beta[:, :, None], value.shape),
        out_gain.reshape(1, size),
    )


def tail_kernel(
    grid,
    merged_ref, tok_ref, gain_ref, wout_hbm, wup_hbm, wdown_hbm,
    out_ref,
    wout, wup, wdown, mg, rs_own, rs_send, rs_recv, gathered, acc,
    y_own, y_send, y_recv, p_send, p_recv, far_total, f_send, f_recv,
    load_sems, own_sem, mg_sems, rs_sems, ghi_sems, gpl_sems, gco_sems, y_sems, p_sems, f_sems,
):
    g = grid
    g.locate()
    n_kv, n_tp, n_lo, n_hi, n_x = g.n_kv, g.n_tp, g.n_lo, g.n_hi, g.n_x
    batch, size = tok_ref.shape
    loads = [
        pltpu.make_async_copy(src, dst, load_sems.at[i])
        for i, (src, dst) in enumerate(((wout_hbm, wout), (wup_hbm, wup), (wdown_hbm, wdown)))
    ]
    for load in loads:
        load.start()
    local = pltpu.make_async_copy(merged_ref, mg.at[g.kv], own_sem)
    local.start()
    kv_peers = [(step(g.kv, k, n_kv), g.tp) for k in range(1, n_kv)]
    tp_peers = [(g.kv, step(g.tp, k, n_tp)) for k in range(1, n_tp)]
    plane_peers = {
        (dy, dx): g.at(g.hi, step(g.lo, dy, n_lo), step(g.x, dx, n_x), g.core)
        for dy, dx in g.plane
    }
    greet(kv_peers + tp_peers + [plane_peers[d] for d in g.plane if d[0] and d[1]])

    started = [
        send(merged_ref, mg.at[g.kv], mg_sems.at[0, k], mg_sems.at[1, k], kv_peers[k - 1])
        for k in range(1, n_kv)
    ]
    loads[0].wait()
    local.wait()
    for copy in started:
        copy.wait()
    rows = mg.shape[1]
    partial = jnp.dot(
        mg[...].reshape(n_kv * rows, mg.shape[2]), wout[...], preferred_element_type=F32
    )
    for t in range(n_tp):
        block = partial[:, t * size : (t + 1) * size]
        rs_own[t] = block
        rs_send[t] = block.astype(BF16)
    started = [
        send(rs_send.at[step(g.tp, k, n_tp)], rs_recv.at[k], rs_sems.at[0, k], rs_sems.at[1, k],
             tp_peers[k - 1])
        for k in range(1, n_tp)
    ]
    branch = rs_own[g.tp]
    for k in range(1, n_tp):
        started[k - 1].wait()
        branch = branch + rs_recv[k].astype(F32)
    residual = (tok_ref[...].astype(F32) + branch).astype(BF16)

    def index(dz, dy, dx, core):
        kv, tp = g.at(step(g.hi, -dz, n_hi), step(g.lo, -dy, n_lo), step(g.x, -dx, n_x), core)
        return kv * n_tp + tp

    mine = index(0, 0, 0, g.core)
    gathered[mine] = residual
    pending = []
    sibling = None if g.n_core == 1 else g.at(g.hi, g.lo, g.x, 1 - g.core)

    def to_sibling(dz, dy, dx):
        if sibling is None:
            return
        place = gathered.at[index(dz, dy, dx, g.core)]
        slot = (dz * n_lo + dy) * n_x + dx
        send(place, place, gco_sems.at[0, slot], gco_sems.at[1, slot], sibling)
        other = gathered.at[index(dz, dy, dx, 1 - g.core)]
        pending.append((place, other, gco_sems.at[0, slot], gco_sems.at[1, slot]))

    def wait_for(src, dst, send_sem, recv_sem, device):
        copy = pltpu.make_async_remote_copy(
            src_ref=src, dst_ref=dst, send_sem=send_sem, recv_sem=recv_sem,
            device_id=device, device_id_type=pl.DeviceIdType.MESH,
        )
        copy.wait_recv()

    sent = []
    own = gathered.at[mine]
    for dz in range(1, n_hi):
        peer = g.at(step(g.hi, dz, n_hi), g.lo, g.x, g.core)
        sent.append(send(own, own, ghi_sems.at[0, dz], ghi_sems.at[1, dz], peer))
    for dz in range(n_hi):
        place = gathered.at[index(dz, 0, 0, g.core)]
        if dz:
            wait_for(own, place, ghi_sems.at[0, dz], ghi_sems.at[1, dz],
                     g.at(step(g.hi, dz, n_hi), g.lo, g.x, g.core))
        for p, d in enumerate(g.plane):
            sent.append(send(place, place, gpl_sems.at[0, dz, p], gpl_sems.at[1, dz, p],
                             plane_peers[d]))
        to_sibling(dz, 0, 0)
    for dz in range(n_hi):
        for p, (dy, dx) in enumerate(g.plane):
            place = gathered.at[index(dz, dy, dx, g.core)]
            wait_for(own, place, gpl_sems.at[0, dz, p], gpl_sems.at[1, dz, p],
                     plane_peers[dy, dx])
            to_sibling(dz, dy, dx)
    for copy in sent:
        copy.wait_send()
    for place, other, send_sem, recv_sem in pending:
        copy = pltpu.make_async_remote_copy(
            src_ref=place, dst_ref=other, send_sem=send_sem, recv_sem=recv_sem,
            device_id=sibling, device_id_type=pl.DeviceIdType.MESH,
        )
        copy.wait_recv()
        copy.wait_send()

    n_dev = n_kv * n_tp
    features = n_dev * size

    def add_squares(i, total):
        block = gathered[i].astype(F32)
        return total + jnp.sum(block * block, axis=1, keepdims=True)

    squares = lax.fori_loop(0, n_dev, add_squares, jnp.zeros((batch, 1), F32))
    scale = lax.rsqrt(squares / features + EPSILON)
    group = n_tp if size % 128 == 0 else 1
    loads[1].wait()
    acc[...] = jnp.zeros_like(acc)

    @pl.loop(0, n_dev // group)
    def _(i):
        parts = [
            (gathered[i * group + j].astype(F32) * scale * gain_ref[i * group + j]).astype(BF16)
            for j in range(group)
        ]
        block = parts[0] if group == 1 else jnp.concatenate(parts, axis=1)
        depth = group * size
        acc[...] += jnp.dot(
            block, wup[pl.ds(pl.multiple_of(i * depth, depth), depth), :],
            preferred_element_type=F32,
        )

    hidden = jnp.square(jnp.maximum(acc[...], 0.0)).astype(BF16)
    loads[2].wait()
    width = n_tp * size

    def down(j):
        columns = pl.ds(pl.multiple_of(j * width, width), width)
        value = jnp.dot(hidden, wdown[:, columns], preferred_element_type=F32)
        for x in range(n_x):
            pair = [
                value[:, (x * g.n_core + c) * size : (x * g.n_core + c + 1) * size]
                for c in range(g.n_core)
            ]
            if g.n_core == 1:
                y_own[j, x] = pair[0]
            else:
                y_own[j, x] = jnp.where(g.core == 0, pair[0], pair[1])
                y_send[j, x] = jnp.where(g.core == 0, pair[1], pair[0]).astype(BF16)

    order = [(dz, dy) for dz in list(range(1, n_hi)) + [0] for dy in range(n_lo)]

    def kv_of(dz, dy):
        return step(g.hi, dz, n_hi) * n_lo + step(g.lo, dy, n_lo)

    swaps = {}
    for s, (dz, dy) in enumerate(order):
        j = kv_of(dz, dy)
        down(j)
        if sibling is not None:
            swaps[dz, dy] = send(y_send.at[j], y_recv.at[j], y_sems.at[0, s], y_sems.at[1, s],
                                 sibling)
    planes = {}
    for dz, dy in order:
        j = kv_of(dz, dy)
        if sibling is not None:
            swaps[dz, dy].wait()
        for dx in range(n_x):
            x = step(g.x, dx, n_x)
            total = y_own[j, x]
            if sibling is not None:
                total = total + y_recv[j, x].astype(F32)
            if (dy, dx) == (0, 0):
                far_total[dz] = total
            else:
                p = g.plane.index((dy, dx))
                p_send[dz, p] = total.astype(BF16)
                planes[dz, p] = send(p_send.at[dz, p], p_recv.at[dz, p], p_sems.at[0, dz, p],
                                     p_sems.at[1, dz, p], plane_peers[dy, dx])
    far = {}
    final = None
    for dz in list(range(1, n_hi)) + [0]:
        total = far_total[dz]
        for p in range(len(g.plane)):
            planes[dz, p].wait()
            total = total + p_recv[dz, p].astype(F32)
        if dz:
            f_send[dz] = total.astype(BF16)
            far[dz] = send(f_send.at[dz], f_recv.at[dz], f_sems.at[0, dz], f_sems.at[1, dz],
                           g.at(step(g.hi, dz, n_hi), g.lo, g.x, g.core))
        else:
            final = total
    for dz in range(1, n_hi):
        far[dz].wait()
        final = final + f_recv[dz].astype(F32)
    out_ref[...] = (gathered[mine].astype(F32) + final).astype(out_ref.dtype)


def tail(grid, merged, tokens, mlp_gain, w_out, w_up, w_down):
    g = grid
    batch, size = tokens.shape
    n_dev = g.n_kv * g.n_tp
    n_plane = max(1, len(g.plane))
    vmem = pl.BlockSpec(memory_space=pltpu.VMEM)
    hbm = pl.BlockSpec(memory_space=pl.ANY)
    dma = pltpu.SemaphoreType.DMA
    block = (batch, size)
    return pl.pallas_call(
        functools.partial(tail_kernel, g),
        out_shape=jax.ShapeDtypeStruct(block, BF16),
        in_specs=[vmem] * 3 + [hbm] * 3,
        out_specs=vmem,
        scratch_shapes=[
            pltpu.VMEM(w_out.shape, BF16),
            pltpu.VMEM(w_up.shape, BF16),
            pltpu.VMEM(w_down.shape, BF16),
            pltpu.VMEM((g.n_kv,) + merged.shape, BF16),
            pltpu.VMEM((g.n_tp,) + block, F32),
            pltpu.VMEM((g.n_tp,) + block, BF16),
            pltpu.VMEM((g.n_tp,) + block, BF16),
            pltpu.VMEM((n_dev,) + block, BF16),
            pltpu.VMEM((batch, w_up.shape[1]), F32),
            pltpu.VMEM((g.n_kv, g.n_x) + block, F32),
            pltpu.VMEM((g.n_kv, g.n_x) + block, BF16),
            pltpu.VMEM((g.n_kv, g.n_x) + block, BF16),
            pltpu.VMEM((g.n_hi, n_plane) + block, BF16),
            pltpu.VMEM((g.n_hi, n_plane) + block, BF16),
            pltpu.VMEM((g.n_hi,) + block, F32),
            pltpu.VMEM((g.n_hi,) + block, BF16),
            pltpu.VMEM((g.n_hi,) + block, BF16),
            dma((3,)),
            dma,
            dma((2, g.n_kv)),
            dma((2, g.n_tp)),
            dma((2, g.n_hi)),
            dma((2, g.n_hi, n_plane)),
            dma((2, g.n_kv * g.n_x)),
            dma((2, g.n_kv)),
            dma((2, g.n_hi, n_plane)),
            dma((2, g.n_hi)),
        ],
        compiler_params=pltpu.CompilerParams(
            collective_id=1, has_side_effects=True, vmem_limit_bytes=VMEM_BYTES
        ),
        name="tail",
    )(merged, tokens, mlp_gain.reshape(n_dev, 1, size), w_out, w_up, w_down)


def head_norm(values):
    return values * lax.rsqrt(jnp.sum(values * values, axis=-1, keepdims=True) + EPSILON)


def local(
    n_kv, n_tp,
    tokens, mix_gain, w_query, w_key, w_value, w_gate, w_beta, w_decay, decay_rate, out_gain,
    state, w_out, mlp_gain, w_up, w_down,
):
    rows, heads, size, _ = state.shape
    all_heads = w_beta.shape[1]
    features = w_query.shape[0] * n_kv
    rate_width = 2 * all_heads
    lanes = -(-(rate_width + 1) // 128) * 128
    w_rates = jnp.concatenate(
        [w_beta, w_decay, jnp.zeros((w_beta.shape[0], lanes - rate_width), w_beta.dtype)], axis=1
    )
    raw, rates = project(
        Grid(n_kv, n_tp), tokens, mix_gain, (w_query, w_key, w_value, w_gate), w_rates, rate_width
    )
    row_scale = lax.rsqrt(rates[:, rate_width : rate_width + 1] / features + EPSILON)
    raw = (raw * row_scale).reshape(4, rows, heads, size)
    query = head_norm(jax.nn.silu(raw[0])) * size ** (-0.5)
    key = head_norm(jax.nn.silu(raw[1]))
    value = jax.nn.silu(raw[2])
    gate = jax.nn.silu(raw[3])
    rates = rates * row_scale
    head_start = lax.axis_index("tp") * heads
    beta = jax.nn.sigmoid(lax.dynamic_slice_in_dim(rates, head_start, heads, 1))
    decay_raw = lax.dynamic_slice_in_dim(rates, all_heads + head_start, heads, 1)
    decay = jnp.exp(-decay_rate[None, :] * jax.nn.softplus(decay_raw))
    new_state, merged = update_state(state, key, query, value, gate, decay, beta, out_gain)
    merged = merged.reshape(rows, heads * size).astype(BF16)
    mixed = tail(Grid(n_kv, n_tp), merged, tokens, mlp_gain, w_out, w_up, w_down)
    return (mixed, new_state)


def solution(mesh):
    placed = (
        P(None, ("kv", "tp")),
        P("kv"),
        P("kv", "tp"),
        P("kv", "tp"),
        P("kv", "tp"),
        P("kv", "tp"),
        P("kv", None),
        P("kv", None),
        P("tp"),
        P(),
        P("kv", "tp", None, None),
        P("tp", "kv"),
        P(),
        P(None, ("kv", "tp")),
        P(("kv", "tp"), None),
    )
    return jax.shard_map(
        functools.partial(local, mesh.shape["kv"], mesh.shape["tp"]),
        mesh=mesh,
        in_specs=placed,
        out_specs=(P(None, ("kv", "tp")), P("kv", "tp", None, None)),
        check_vma=False,
    )
```

```python
import functools
import math

import jax
import jax.numpy as jnp
from jax import lax
from jax.experimental import pallas as pl
from jax.experimental.pallas import tpu as pltpu
from jax.sharding import PartitionSpec as P

EPSILON = 1e-06
CORES = 2
VMEM_BYTES = 60 * 2**20
BF16 = jnp.bfloat16
F32 = jnp.float32


class Grid:
    def __init__(self, n_kv, n_tp):
        self.n_kv, self.n_tp = n_kv, n_tp
        low = max(f for f in range(1, math.isqrt(n_kv) + 1) if n_kv % f == 0)
        self.n_lo, self.n_hi = low, n_kv // low
        self.n_core = CORES if n_tp % CORES == 0 else 1
        self.n_x = n_tp // self.n_core
        self.plane = [
            (dy, dx) for dy in range(self.n_lo) for dx in range(self.n_x) if (dy, dx) != (0, 0)
        ]

    def locate(self):
        self.kv, self.tp = lax.axis_index("kv"), lax.axis_index("tp")
        self.hi, self.lo = self.kv // self.n_lo, lax.rem(self.kv, self.n_lo)
        self.x, self.core = self.tp // self.n_core, lax.rem(self.tp, self.n_core)

    def at(self, hi, lo, x, core):
        return (hi * self.n_lo + lo, x * self.n_core + core)


def step(index, offset, size):
    return lax.rem(index + (offset % size), size) if offset % size else index


def send(src, dst, send_sem, recv_sem, device):
    copy = pltpu.make_async_remote_copy(
        src_ref=src,
        dst_ref=dst,
        send_sem=send_sem,
        recv_sem=recv_sem,
        device_id=device,
        device_id_type=pl.DeviceIdType.MESH,
    )
    copy.start()
    return copy


def silu(values):
    return values / (1.0 + jnp.exp(-values))


def layer_kernel(
    grid, all_heads, lane_gap, features,
    tok_ref, mix_ref, wb_ref, wd_ref, rate_ref, out_gain_ref, gain_ref,
    wk_hbm, wq_hbm, wv_hbm, wg_hbm, state_hbm, wout_hbm, wup_hbm, wdown_hbm,
    out_ref, key_ref, change_ref, decay_ref,
    cols, w_mix, w_rates, part, rate_part, rate_recv,
    near_send, near_recv, far_total, far_send, far_recv,
    state, query_buf, value_buf, gate_buf, recalled, echoed,
    wout, wup, wdown, mg, rs_own, rs_send, rs_recv, gathered, acc,
    y_own, y_send, y_recv, p_send, p_recv, last_total, f_send, f_recv,
    mix_load_sems, load_sems, own_sem, tok_sems, rate_sems, near_sems, far_sems,
    mg_sems, rs_sems, ghi_sems, gpl_sems, gco_sems, y_sems, p_sems, f_sems,
):
    g = grid
    g.locate()
    n_kv, n_tp, n_lo, n_hi, n_x = g.n_kv, g.n_tp, g.n_lo, g.n_hi, g.n_x
    batch, size = tok_ref.shape
    heads, rows, head_size = key_ref.shape
    own_cols = pltpu.make_async_copy(tok_ref, cols.at[g.tp], own_sem)
    own_cols.start()
    kv_peers = [(step(g.kv, k, n_kv), g.tp) for k in range(1, n_kv)]
    tp_peers = [(g.kv, step(g.tp, k, n_tp)) for k in range(1, n_tp)]
    plane_peers = {
        (dy, dx): g.at(g.hi, step(g.lo, dy, n_lo), step(g.x, dx, n_x), g.core)
        for dy, dx in g.plane
    }
    barrier = pltpu.get_barrier_semaphore()
    everyone = kv_peers + tp_peers + [plane_peers[d] for d in g.plane if d[0] and d[1]]
    for peer in everyone:
        pl.semaphore_signal(barrier, inc=1, device_id=peer, device_id_type=pl.DeviceIdType.MESH)
    mix_loads = [
        pltpu.make_async_copy(w, w_mix.at[c], mix_load_sems.at[c])
        for c, w in enumerate((wk_hbm, wq_hbm, wv_hbm, wg_hbm))
    ]
    loads = [
        pltpu.make_async_copy(a, b, load_sems.at[i])
        for i, (a, b) in enumerate(
            ((wout_hbm, wout), (wup_hbm, wup), (wdown_hbm, wdown), (state_hbm, state))
        )
    ]
    for load in mix_loads + [loads[3]] + loads[:3]:
        load.start()
    w_rates[...] = jnp.zeros_like(w_rates)
    w_rates[0:all_heads, :] = wb_ref[...]
    w_rates[lane_gap : lane_gap + all_heads, :] = wd_ref[...]
    pl.semaphore_wait(barrier, len(everyone))

    started = [
        send(tok_ref, cols.at[g.tp], tok_sems.at[0, k], tok_sems.at[1, k], tp_peers[k - 1])
        for k in range(1, n_tp)
    ]
    own_cols.wait()
    for copy in started:
        copy.wait()
    blocks = [cols[i].astype(F32) for i in range(n_tp)]
    squares = sum(jnp.sum(b * b, axis=1, keepdims=True) for b in blocks)
    normed = [(blocks[i] * mix_ref[i]).astype(BF16) for i in range(n_tp)]
    if size % 128 == 0:
        normed = [jnp.concatenate(normed, axis=1)]
    depth = normed[0].shape[1]

    rates = sum(
        lax.dot_general(
            normed[i], w_rates[:, i * depth : (i + 1) * depth], (((1,), (1,)), ((), ())),
            preferred_element_type=F32,
        )
        for i in range(len(normed))
    )
    lane = lax.broadcasted_iota(jnp.int32, rates.shape, 1)
    rates = jnp.where(lane == 2 * lane_gap, squares, rates)
    rate_part[...] = rates.reshape(n_kv, rows, rates.shape[1])
    rate_copies = [
        send(rate_part.at[step(g.kv, k, n_kv)], rate_recv.at[k], rate_sems.at[0, k],
             rate_sems.at[1, k], kv_peers[k - 1])
        for k in range(1, n_kv)
    ]
    near = {}
    for c in range(4):
        mix_loads[c].wait()
        value = sum(
            jnp.dot(normed[i], w_mix[c, i * depth : (i + 1) * depth, :],
                    preferred_element_type=F32)
            for i in range(len(normed))
        ).reshape(n_kv, rows, w_mix.shape[2])
        part[c] = value
        for lo in range(n_lo):
            for hi in range(n_hi):
                near_send[c, lo, hi] = value[hi * n_lo + lo].astype(BF16)
        for k in range(1, n_lo):
            lo = step(g.lo, k, n_lo)
            near[c, k] = send(near_send.at[c, lo], near_recv.at[c, k], near_sems.at[0, c, k],
                              near_sems.at[1, c, k], (g.hi * n_lo + lo, g.tp))
    far = {}
    for c in range(4):
        for k in range(1, n_lo):
            near[c, k].wait()
        for d in list(range(1, n_hi)) + [0]:
            hi = step(g.hi, d, n_hi)
            total = part[c, hi * n_lo + g.lo]
            for k in range(1, n_lo):
                total = total + near_recv[c, k, hi].astype(F32)
            if d == 0:
                far_total[c] = total
            else:
                far_send[c, d] = total.astype(BF16)
                far[c, d] = send(far_send.at[c, d], far_recv.at[c, d], far_sems.at[0, c, d],
                                 far_sems.at[1, c, d], (hi * n_lo + g.lo, g.tp))
    for copy in rate_copies:
        copy.wait()
    rates = rate_part[g.kv]
    for k in range(1, n_kv):
        rates = rates + rate_recv[k]
    lane = lax.broadcasted_iota(jnp.int32, rates.shape, 1)

    def pick(index):
        return jnp.sum(jnp.where(lane == index, rates, 0.0), axis=1, keepdims=True)

    row_scale = lax.rsqrt(pick(2 * lane_gap) / features + EPSILON)

    def arrived(c):
        total = far_total[c]
        for d in range(1, n_hi):
            far[c, d].wait()
            total = total + far_recv[c, d].astype(F32)
        return silu(total * row_scale)

    def unit(values):
        return values * lax.rsqrt(jnp.sum(values * values, axis=1, keepdims=True) + EPSILON)

    def of_head(values, h):
        return values[:, h * head_size : (h + 1) * head_size]

    keys = arrived(0)
    for h in range(heads):
        key_ref[h] = unit(of_head(keys, h))
    queries = arrived(1)
    for h in range(heads):
        query_buf[h] = unit(of_head(queries, h)) * head_size ** (-0.5)
    loads[3].wait()

    @pl.loop(0, heads)
    def _(h):
        tall_key, tall_query = key_ref[h].T, query_buf[h].T
        for r in range(rows):
            block = state[r, h]
            recalled[h, r : r + 1, :] = jnp.sum(
                block * tall_key[:, r : r + 1], axis=0, keepdims=True
            )
            echoed[h, r : r + 1, :] = jnp.sum(
                block * tall_query[:, r : r + 1], axis=0, keepdims=True
            )

    value_buf[...] = arrived(2)
    gate_buf[...] = arrived(3)
    head_start = g.tp * heads
    own_merged = mg.at[g.kv]
    for h in range(heads):
        beta = 1.0 / (1.0 + jnp.exp(-(pick(head_start + h) * row_scale)))
        decay_raw = pick(head_start + (lane_gap + h)) * row_scale
        softplus = jnp.maximum(decay_raw, 0.0) + jnp.log1p(jnp.exp(-jnp.abs(decay_raw)))
        decay = jnp.exp(-(rate_ref[:, h : h + 1] * softplus))
        change = beta * (of_head(value_buf, h) - decay * recalled[h])
        overlap = jnp.sum(key_ref[h] * query_buf[h], axis=1, keepdims=True)
        readout = decay * echoed[h] + overlap * change
        change_ref[h] = change
        decay_ref[h] = jnp.broadcast_to(decay, change.shape)
        scaled = (
            readout
            * lax.rsqrt(jnp.mean(readout * readout, axis=1, keepdims=True) + EPSILON)
            * out_gain_ref[...]
        )
        own_merged[:, h * head_size : (h + 1) * head_size] = (
            scaled * of_head(gate_buf, h)
        ).astype(BF16)

    started = [
        send(own_merged, own_merged, mg_sems.at[0, k], mg_sems.at[1, k], kv_peers[k - 1])
        for k in range(1, n_kv)
    ]
    loads[0].wait()
    for k in range(1, n_kv):
        started[k - 1].wait_send()
        pltpu.make_async_remote_copy(
            src_ref=own_merged, dst_ref=mg.at[step(g.kv, -k, n_kv)], send_sem=mg_sems.at[0, k],
            recv_sem=mg_sems.at[1, k], device_id=kv_peers[k - 1],
            device_id_type=pl.DeviceIdType.MESH,
        ).wait_recv()
    partial = jnp.dot(
        mg[...].reshape(n_kv * rows, mg.shape[2]), wout[...], preferred_element_type=F32
    )
    for t in range(n_tp):
        block = partial[:, t * size : (t + 1) * size]
        rs_own[t] = block
        rs_send[t] = block.astype(BF16)
    started = [
        send(rs_send.at[step(g.tp, k, n_tp)], rs_recv.at[k], rs_sems.at[0, k], rs_sems.at[1, k],
             tp_peers[k - 1])
        for k in range(1, n_tp)
    ]
    branch = rs_own[g.tp]
    for k in range(1, n_tp):
        started[k - 1].wait()
        branch = branch + rs_recv[k].astype(F32)
    residual = (tok_ref[...].astype(F32) + branch).astype(BF16)

    def index(dz, dy, dx, core):
        kv, tp = g.at(step(g.hi, -dz, n_hi), step(g.lo, -dy, n_lo), step(g.x, -dx, n_x), core)
        return kv * n_tp + tp

    mine = index(0, 0, 0, g.core)
    gathered[mine] = residual
    pending = []
    sibling = None if g.n_core == 1 else g.at(g.hi, g.lo, g.x, 1 - g.core)

    def to_sibling(dz, dy, dx):
        if sibling is None:
            return
        place = gathered.at[index(dz, dy, dx, g.core)]
        slot = (dz * n_lo + dy) * n_x + dx
        send(place, place, gco_sems.at[0, slot], gco_sems.at[1, slot], sibling)
        other = gathered.at[index(dz, dy, dx, 1 - g.core)]
        pending.append((place, other, gco_sems.at[0, slot], gco_sems.at[1, slot]))

    def wait_for(src, dst, send_sem, recv_sem, device):
        copy = pltpu.make_async_remote_copy(
            src_ref=src, dst_ref=dst, send_sem=send_sem, recv_sem=recv_sem,
            device_id=device, device_id_type=pl.DeviceIdType.MESH,
        )
        copy.wait_recv()

    sent = []
    own = gathered.at[mine]
    for dz in range(1, n_hi):
        peer = g.at(step(g.hi, dz, n_hi), g.lo, g.x, g.core)
        sent.append(send(own, own, ghi_sems.at[0, dz], ghi_sems.at[1, dz], peer))
    for dz in range(n_hi):
        place = gathered.at[index(dz, 0, 0, g.core)]
        if dz:
            wait_for(own, place, ghi_sems.at[0, dz], ghi_sems.at[1, dz],
                     g.at(step(g.hi, dz, n_hi), g.lo, g.x, g.core))
        for p, d in enumerate(g.plane):
            sent.append(send(place, place, gpl_sems.at[0, dz, p], gpl_sems.at[1, dz, p],
                             plane_peers[d]))
        to_sibling(dz, 0, 0)
    for dz in range(n_hi):
        for p, (dy, dx) in enumerate(g.plane):
            place = gathered.at[index(dz, dy, dx, g.core)]
            wait_for(own, place, gpl_sems.at[0, dz, p], gpl_sems.at[1, dz, p],
                     plane_peers[dy, dx])
            to_sibling(dz, dy, dx)
    for copy in sent:
        copy.wait_send()
    for place, other, send_sem, recv_sem in pending:
        copy = pltpu.make_async_remote_copy(
            src_ref=place, dst_ref=other, send_sem=send_sem, recv_sem=recv_sem,
            device_id=sibling, device_id_type=pl.DeviceIdType.MESH,
        )
        copy.wait_recv()
        copy.wait_send()

    n_dev = n_kv * n_tp

    def add_squares(i, total):
        block = gathered[i].astype(F32)
        return total + jnp.sum(block * block, axis=1, keepdims=True)

    squares = lax.fori_loop(0, n_dev, add_squares, jnp.zeros((batch, 1), F32))
    scale = lax.rsqrt(squares / features + EPSILON)
    group = n_tp if size % 128 == 0 else 1
    loads[1].wait()
    acc[...] = jnp.zeros_like(acc)

    @pl.loop(0, n_dev // group)
    def _(i):
        parts = [
            (gathered[i * group + j].astype(F32) * scale * gain_ref[i * group + j]).astype(BF16)
            for j in range(group)
        ]
        block = parts[0] if group == 1 else jnp.concatenate(parts, axis=1)
        depth = group * size
        acc[...] += jnp.dot(
            block, wup[pl.ds(pl.multiple_of(i * depth, depth), depth), :],
            preferred_element_type=F32,
        )

    hidden = jnp.square(jnp.maximum(acc[...], 0.0)).astype(BF16)
    loads[2].wait()
    width = n_tp * size

    def down(j):
        columns = pl.ds(pl.multiple_of(j * width, width), width)
        value = jnp.dot(hidden, wdown[:, columns], preferred_element_type=F32)
        for x in range(n_x):
            pair = [
                value[:, (x * g.n_core + c) * size : (x * g.n_core + c + 1) * size]
                for c in range(g.n_core)
            ]
            if g.n_core == 1:
                y_own[j, x] = pair[0]
            else:
                y_own[j, x] = jnp.where(g.core == 0, pair[0], pair[1])
                y_send[j, x] = jnp.where(g.core == 0, pair[1], pair[0]).astype(BF16)

    order = [(dz, dy) for dz in list(range(1, n_hi)) + [0] for dy in range(n_lo)]

    def kv_of(dz, dy):
        return step(g.hi, dz, n_hi) * n_lo + step(g.lo, dy, n_lo)

    swaps = {}
    for s, (dz, dy) in enumerate(order):
        j = kv_of(dz, dy)
        down(j)
        if sibling is not None:
            swaps[dz, dy] = send(y_send.at[j], y_recv.at[j], y_sems.at[0, s], y_sems.at[1, s],
                                 sibling)
    planes = {}
    for dz, dy in order:
        j = kv_of(dz, dy)
        if sibling is not None:
            swaps[dz, dy].wait()
        for dx in range(n_x):
            x = step(g.x, dx, n_x)
            total = y_own[j, x]
            if sibling is not None:
                total = total + y_recv[j, x].astype(F32)
            if (dy, dx) == (0, 0):
                last_total[dz] = total
            else:
                p = g.plane.index((dy, dx))
                p_send[dz, p] = total.astype(BF16)
                planes[dz, p] = send(p_send.at[dz, p], p_recv.at[dz, p], p_sems.at[0, dz, p],
                                     p_sems.at[1, dz, p], plane_peers[dy, dx])
    last = {}
    final = None
    for dz in list(range(1, n_hi)) + [0]:
        total = last_total[dz]
        for p in range(len(g.plane)):
            planes[dz, p].wait()
            total = total + p_recv[dz, p].astype(F32)
        if dz:
            f_send[dz] = total.astype(BF16)
            last[dz] = send(f_send.at[dz], f_recv.at[dz], f_sems.at[0, dz], f_sems.at[1, dz],
                           g.at(step(g.hi, dz, n_hi), g.lo, g.x, g.core))
        else:
            final = total
    for dz in range(1, n_hi):
        last[dz].wait()
        final = final + f_recv[dz].astype(F32)
    out_ref[...] = (gathered[mine].astype(F32) + final).astype(out_ref.dtype)


def layer(grid, tokens, mix_gain, weights, w_beta, w_decay, decay_rate, out_gain, state, w_out,
          mlp_gain, w_up, w_down):
    g = grid
    batch, size = tokens.shape
    n_dev = g.n_kv * g.n_tp
    rows, heads, head_size, _ = state.shape
    depth, width = weights[0].shape
    all_heads = w_beta.shape[1]
    lane_gap = -(-all_heads // 32) * 32
    lanes = -(-(2 * lane_gap + 1) // 128) * 128
    n_plane = max(1, len(g.plane))
    vmem = pl.BlockSpec(memory_space=pltpu.VMEM)
    hbm = pl.BlockSpec(memory_space=pl.ANY)
    dma = pltpu.SemaphoreType.DMA
    block = (batch, size)
    per_head = (heads, rows, head_size)
    return pl.pallas_call(
        functools.partial(layer_kernel, g, all_heads, lane_gap, n_dev * size),
        out_shape=(
            jax.ShapeDtypeStruct(block, BF16),
            jax.ShapeDtypeStruct(per_head, F32),
            jax.ShapeDtypeStruct(per_head, F32),
            jax.ShapeDtypeStruct(per_head, F32),
        ),
        in_specs=[vmem] * 7 + [hbm] * 8,
        out_specs=(vmem,) * 4,
        scratch_shapes=[
            pltpu.VMEM((g.n_tp,) + block, BF16),
            pltpu.VMEM((4, depth, width), BF16),
            pltpu.VMEM((lanes, depth), BF16),
            pltpu.VMEM((4, g.n_kv, rows, width), F32),
            pltpu.VMEM((g.n_kv, rows, lanes), F32),
            pltpu.VMEM((g.n_kv, rows, lanes), F32),
            pltpu.VMEM((4, g.n_lo, g.n_hi, rows, width), BF16),
            pltpu.VMEM((4, g.n_lo, g.n_hi, rows, width), BF16),
            pltpu.VMEM((4, rows, width), F32),
            pltpu.VMEM((4, g.n_hi, rows, width), BF16),
            pltpu.VMEM((4, g.n_hi, rows, width), BF16),
            pltpu.VMEM(state.shape, F32),
            pltpu.VMEM(per_head, F32),
            pltpu.VMEM((rows, width), F32),
            pltpu.VMEM((rows, width), F32),
            pltpu.VMEM(per_head, F32),
            pltpu.VMEM(per_head, F32),
            pltpu.VMEM(w_out.shape, BF16),
            pltpu.VMEM(w_up.shape, BF16),
            pltpu.VMEM(w_down.shape, BF16),
            pltpu.VMEM((g.n_kv, rows, width), BF16),
            pltpu.VMEM((g.n_tp,) + block, F32),
            pltpu.VMEM((g.n_tp,) + block, BF16),
            pltpu.VMEM((g.n_tp,) + block, BF16),
            pltpu.VMEM((n_dev,) + block, BF16),
            pltpu.VMEM((batch, w_up.shape[1]), F32),
            pltpu.VMEM((g.n_kv, g.n_x) + block, F32),
            pltpu.VMEM((g.n_kv, g.n_x) + block, BF16),
            pltpu.VMEM((g.n_kv, g.n_x) + block, BF16),
            pltpu.VMEM((g.n_hi, n_plane) + block, BF16),
            pltpu.VMEM((g.n_hi, n_plane) + block, BF16),
            pltpu.VMEM((g.n_hi,) + block, F32),
            pltpu.VMEM((g.n_hi,) + block, BF16),
            pltpu.VMEM((g.n_hi,) + block, BF16),
            dma((4,)),
            dma((4,)),
            dma,
            dma((2, g.n_tp)),
            dma((2, g.n_kv)),
            dma((2, 4, g.n_lo)),
            dma((2, 4, g.n_hi)),
            dma((2, g.n_kv)),
            dma((2, g.n_tp)),
            dma((2, g.n_hi)),
            dma((2, g.n_hi, n_plane)),
            dma((2, g.n_kv * g.n_x)),
            dma((2, g.n_kv)),
            dma((2, g.n_hi, n_plane)),
            dma((2, g.n_hi)),
        ],
        compiler_params=pltpu.CompilerParams(
            collective_id=0, has_side_effects=True, vmem_limit_bytes=VMEM_BYTES
        ),
        name="layer",
    )(
        tokens, mix_gain.reshape(g.n_tp, 1, size), w_beta.T, w_decay.T,
        decay_rate.reshape(1, heads), out_gain.reshape(1, head_size),
        mlp_gain.reshape(n_dev, 1, size), *weights, state, w_out, w_up, w_down,
    )


def state_kernel(state_ref, key_ref, change_ref, decay_ref, new_ref):
    tall = key_ref[0].T
    for r in range(state_ref.shape[0]):
        row = slice(r, r + 1)
        new_ref[r, 0] = (
            state_ref[r, 0] * decay_ref[0, row, :] + tall[:, row] * change_ref[0, row, :]
        )


def write_state(state, key, change, decay):
    rows, heads, size, _ = state.shape
    whole = pl.BlockSpec((rows, 1, size, size), lambda i: (0, i, 0, 0))
    small = pl.BlockSpec((1, rows, size), lambda i: (i, 0, 0))
    return pl.pallas_call(
        state_kernel,
        grid=(heads,),
        out_shape=jax.ShapeDtypeStruct(state.shape, F32),
        in_specs=[whole, small, small, small],
        out_specs=whole,
        compiler_params=pltpu.CompilerParams(dimension_semantics=("arbitrary",)),
        name="state",
    )(state, key, change, decay)


def local(
    n_kv, n_tp,
    tokens, mix_gain, w_query, w_key, w_value, w_gate, w_beta, w_decay, decay_rate, out_gain,
    state, w_out, mlp_gain, w_up, w_down,
):
    mixed, key, change, decay = layer(
        Grid(n_kv, n_tp), tokens, mix_gain, (w_key, w_query, w_value, w_gate), w_beta, w_decay,
        decay_rate, out_gain, state, w_out, mlp_gain, w_up, w_down,
    )
    return (mixed, write_state(state, key, change, decay))


def solution(mesh):
    placed = (
        P(None, ("kv", "tp")),
        P("kv"),
        P("kv", "tp"),
        P("kv", "tp"),
        P("kv", "tp"),
        P("kv", "tp"),
        P("kv", None),
        P("kv", None),
        P("tp"),
        P(),
        P("kv", "tp", None, None),
        P("tp", "kv"),
        P(),
        P(None, ("kv", "tp")),
        P(("kv", "tp"), None),
    )
    return jax.shard_map(
        functools.partial(local, mesh.shape["kv"], mesh.shape["tp"]),
        mesh=mesh,
        in_specs=placed,
        out_specs=(P(None, ("kv", "tp")), P("kv", "tp", None, None)),
        check_vma=False,
    )
```

```python
import functools
import math

import jax
import jax.numpy as jnp
from jax import lax
from jax.experimental import pallas as pl
from jax.experimental.pallas import tpu as pltpu
from jax.sharding import PartitionSpec as P

EPSILON = 1e-06
CORES = 2
VMEM_BYTES = 67043328
SPARE_BYTES = 2**19
BF16 = jnp.bfloat16
F32 = jnp.float32


class Grid:
    def __init__(self, n_kv, n_tp):
        self.n_kv, self.n_tp = n_kv, n_tp
        low = max(f for f in range(1, math.isqrt(n_kv) + 1) if n_kv % f == 0)
        self.n_lo, self.n_hi = low, n_kv // low
        self.n_core = CORES if n_tp % CORES == 0 else 1
        self.n_x = n_tp // self.n_core
        self.plane = [
            (dy, dx) for dy in range(self.n_lo) for dx in range(self.n_x) if (dy, dx) != (0, 0)
        ]

    def locate(self):
        self.kv, self.tp = lax.axis_index("kv"), lax.axis_index("tp")
        self.hi, self.lo = self.kv // self.n_lo, lax.rem(self.kv, self.n_lo)
        self.x, self.core = self.tp // self.n_core, lax.rem(self.tp, self.n_core)

    def at(self, hi, lo, x, core):
        return (hi * self.n_lo + lo, x * self.n_core + core)


def step(index, offset, size):
    return lax.rem(index + (offset % size), size) if offset % size else index


def padded_bytes(shape, dtype):
    rows, lanes = -(-shape[-2] // 16) * 16, -(-shape[-1] // 128) * 128
    return math.prod(shape[:-2]) * rows * lanes * jnp.dtype(dtype).itemsize


def send(src, dst, send_sem, recv_sem, device):
    copy = pltpu.make_async_remote_copy(
        src_ref=src,
        dst_ref=dst,
        send_sem=send_sem,
        recv_sem=recv_sem,
        device_id=device,
        device_id_type=pl.DeviceIdType.MESH,
    )
    copy.start()
    return copy


def silu(values):
    return values / (1.0 + jnp.exp(-values))


def layer_kernel(
    grid, all_heads, lane_gap, features,
    tok_ref, mix_ref, wb_ref, wd_ref, rate_ref, out_gain_ref, gain_ref,
    wk_hbm, wq_hbm, wv_hbm, wg_hbm, state_hbm, wout_hbm, wup_hbm, wdown_hbm,
    out_ref, new_ref,
    cols, w_mix, w_rates, part, rate_part, rate_recv,
    near_send, near_recv, far_total, far_send, far_recv,
    state, key_ref, change_ref, decay_ref, query_buf, value_buf, gate_buf, recalled, echoed,
    wout, wup, wdown, mg, rs_own, rs_send, rs_recv, gathered, acc, squares_ref,
    y_own, y_send, y_recv, p_send, p_recv, last_total, f_send, f_recv,
    mix_load_sems, load_sems, own_sem, tok_sems, rate_sems, near_sems, far_sems,
    mg_sems, rs_sems, ghi_sems, gpl_sems, gco_sems, y_sems, p_sems, f_sems,
):
    g = grid
    g.locate()
    n_kv, n_tp, n_lo, n_hi, n_x = g.n_kv, g.n_tp, g.n_lo, g.n_hi, g.n_x
    batch, size = tok_ref.shape
    heads, rows, head_size = key_ref.shape
    own_cols = pltpu.make_async_copy(tok_ref, cols.at[g.tp], own_sem)
    own_cols.start()
    kv_peers = [(step(g.kv, k, n_kv), g.tp) for k in range(1, n_kv)]
    tp_peers = [(g.kv, step(g.tp, k, n_tp)) for k in range(1, n_tp)]
    plane_peers = {
        (dy, dx): g.at(g.hi, step(g.lo, dy, n_lo), step(g.x, dx, n_x), g.core)
        for dy, dx in g.plane
    }
    barrier = pltpu.get_barrier_semaphore()
    everyone = kv_peers + tp_peers + [plane_peers[d] for d in g.plane if d[0] and d[1]]
    for peer in everyone:
        pl.semaphore_signal(barrier, inc=1, device_id=peer, device_id_type=pl.DeviceIdType.MESH)
    mix_loads = [
        pltpu.make_async_copy(w, w_mix.at[c], mix_load_sems.at[c])
        for c, w in enumerate((wk_hbm, wq_hbm, wv_hbm, wg_hbm))
    ]
    loads = [
        pltpu.make_async_copy(a, b, load_sems.at[i])
        for i, (a, b) in enumerate(
            ((wout_hbm, wout), (wup_hbm, wup), (wdown_hbm, wdown), (state_hbm, state))
        )
    ]
    for load in mix_loads + [loads[3]] + loads[:3]:
        load.start()
    w_rates[...] = jnp.zeros_like(w_rates)
    w_rates[0:all_heads, :] = wb_ref[...]
    w_rates[lane_gap : lane_gap + all_heads, :] = wd_ref[...]
    pl.semaphore_wait(barrier, len(everyone))

    started = [
        send(tok_ref, cols.at[g.tp], tok_sems.at[0, k], tok_sems.at[1, k], tp_peers[k - 1])
        for k in range(1, n_tp)
    ]
    own_cols.wait()
    for copy in started:
        copy.wait()
    blocks = [cols[i].astype(F32) for i in range(n_tp)]
    squares = sum(jnp.sum(b * b, axis=1, keepdims=True) for b in blocks)
    normed = [(blocks[i] * mix_ref[i]).astype(BF16) for i in range(n_tp)]
    if size % 128 == 0:
        normed = [jnp.concatenate(normed, axis=1)]
    depth = normed[0].shape[1]

    rates = sum(
        lax.dot_general(
            normed[i], w_rates[:, i * depth : (i + 1) * depth], (((1,), (1,)), ((), ())),
            preferred_element_type=F32,
        )
        for i in range(len(normed))
    )
    lane = lax.broadcasted_iota(jnp.int32, rates.shape, 1)
    rates = jnp.where(lane == 2 * lane_gap, squares, rates)
    rate_part[...] = rates.reshape(n_kv, rows, rates.shape[1])
    rate_copies = [
        send(rate_part.at[step(g.kv, k, n_kv)], rate_recv.at[k], rate_sems.at[0, k],
             rate_sems.at[1, k], kv_peers[k - 1])
        for k in range(1, n_kv)
    ]
    near = {}
    for c in range(4):
        mix_loads[c].wait()
        value = sum(
            jnp.dot(normed[i], w_mix[c, i * depth : (i + 1) * depth, :],
                    preferred_element_type=F32)
            for i in range(len(normed))
        ).reshape(n_kv, rows, w_mix.shape[2])
        part[c] = value
        for lo in range(n_lo):
            for hi in range(n_hi):
                near_send[c, lo, hi] = value[hi * n_lo + lo].astype(BF16)
        for k in range(1, n_lo):
            lo = step(g.lo, k, n_lo)
            near[c, k] = send(near_send.at[c, lo], near_recv.at[c, k], near_sems.at[0, c, k],
                              near_sems.at[1, c, k], (g.hi * n_lo + lo, g.tp))
    far = {}
    for c in range(4):
        for k in range(1, n_lo):
            near[c, k].wait()
        for d in list(range(1, n_hi)) + [0]:
            hi = step(g.hi, d, n_hi)
            total = part[c, hi * n_lo + g.lo]
            for k in range(1, n_lo):
                total = total + near_recv[c, k, hi].astype(F32)
            if d == 0:
                far_total[c] = total
            else:
                far_send[c, d] = total.astype(BF16)
                far[c, d] = send(far_send.at[c, d], far_recv.at[c, d], far_sems.at[0, c, d],
                                 far_sems.at[1, c, d], (hi * n_lo + g.lo, g.tp))
    for copy in rate_copies:
        copy.wait()
    rates = rate_part[g.kv]
    for k in range(1, n_kv):
        rates = rates + rate_recv[k]
    lane = lax.broadcasted_iota(jnp.int32, rates.shape, 1)

    def pick(index):
        return jnp.sum(jnp.where(lane == index, rates, 0.0), axis=1, keepdims=True)

    row_scale = lax.rsqrt(pick(2 * lane_gap) / features + EPSILON)

    def arrived(c):
        total = far_total[c]
        for d in range(1, n_hi):
            far[c, d].wait()
            total = total + far_recv[c, d].astype(F32)
        return silu(total * row_scale)

    def unit(values):
        return values * lax.rsqrt(jnp.sum(values * values, axis=1, keepdims=True) + EPSILON)

    def of_head(values, h):
        return values[:, h * head_size : (h + 1) * head_size]

    keys = arrived(0)
    for h in range(heads):
        key_ref[h] = unit(of_head(keys, h))
    queries = arrived(1)
    for h in range(heads):
        query_buf[h] = unit(of_head(queries, h)) * head_size ** (-0.5)
    loads[3].wait()

    @pl.loop(0, heads)
    def _(h):
        tall_key, tall_query = key_ref[h].T, query_buf[h].T
        for r in range(rows):
            block = state[r, h]
            recalled[h, r : r + 1, :] = jnp.sum(
                block * tall_key[:, r : r + 1], axis=0, keepdims=True
            )
            echoed[h, r : r + 1, :] = jnp.sum(
                block * tall_query[:, r : r + 1], axis=0, keepdims=True
            )

    value_buf[...] = arrived(2)
    gate_buf[...] = arrived(3)
    head_start = g.tp * heads
    own_merged = mg.at[g.kv]
    for h in range(heads):
        beta = 1.0 / (1.0 + jnp.exp(-(pick(head_start + h) * row_scale)))
        decay_raw = pick(head_start + (lane_gap + h)) * row_scale
        softplus = jnp.maximum(decay_raw, 0.0) + jnp.log1p(jnp.exp(-jnp.abs(decay_raw)))
        decay = jnp.exp(-(rate_ref[:, h : h + 1] * softplus))
        change = beta * (of_head(value_buf, h) - decay * recalled[h])
        overlap = jnp.sum(key_ref[h] * query_buf[h], axis=1, keepdims=True)
        readout = decay * echoed[h] + overlap * change
        change_ref[h] = change
        decay_ref[h] = jnp.broadcast_to(decay, change.shape)
        scaled = (
            readout
            * lax.rsqrt(jnp.mean(readout * readout, axis=1, keepdims=True) + EPSILON)
            * out_gain_ref[...]
        )
        own_merged[:, h * head_size : (h + 1) * head_size] = (
            scaled * of_head(gate_buf, h)
        ).astype(BF16)

    started = [
        send(own_merged, own_merged, mg_sems.at[0, k], mg_sems.at[1, k], kv_peers[k - 1])
        for k in range(1, n_kv)
    ]

    @pl.loop(0, heads)
    def _(h):
        tall = key_ref[h].T
        for r in range(rows):
            row = slice(r, r + 1)
            new_ref[r, h] = (
                state[r, h] * decay_ref[h, row, :] + tall[:, row] * change_ref[h, row, :]
            )

    loads[0].wait()
    for k in range(1, n_kv):
        started[k - 1].wait_send()
        pltpu.make_async_remote_copy(
            src_ref=own_merged, dst_ref=mg.at[step(g.kv, -k, n_kv)], send_sem=mg_sems.at[0, k],
            recv_sem=mg_sems.at[1, k], device_id=kv_peers[k - 1],
            device_id_type=pl.DeviceIdType.MESH,
        ).wait_recv()
    partial = jnp.dot(
        mg[...].reshape(n_kv * rows, mg.shape[2]), wout[...], preferred_element_type=F32
    )
    for t in range(n_tp):
        block = partial[:, t * size : (t + 1) * size]
        rs_own[t] = block
        rs_send[t] = block.astype(BF16)
    started = [
        send(rs_send.at[step(g.tp, k, n_tp)], rs_recv.at[k], rs_sems.at[0, k], rs_sems.at[1, k],
             tp_peers[k - 1])
        for k in range(1, n_tp)
    ]
    branch = rs_own[g.tp]
    for k in range(1, n_tp):
        started[k - 1].wait()
        branch = branch + rs_recv[k].astype(F32)
    residual = (tok_ref[...].astype(F32) + branch).astype(BF16)

    def index(dz, dy, dx, core):
        kv, tp = g.at(step(g.hi, -dz, n_hi), step(g.lo, -dy, n_lo), step(g.x, -dx, n_x), core)
        return kv * n_tp + tp

    mine = index(0, 0, 0, g.core)
    gathered[mine] = residual
    pending = []
    sibling = None if g.n_core == 1 else g.at(g.hi, g.lo, g.x, 1 - g.core)

    def to_sibling(dz, dy, dx):
        if sibling is None:
            return
        place = gathered.at[index(dz, dy, dx, g.core)]
        slot = (dz * n_lo + dy) * n_x + dx
        send(place, place, gco_sems.at[0, slot], gco_sems.at[1, slot], sibling)
        other = gathered.at[index(dz, dy, dx, 1 - g.core)]
        pending.append((place, other, index(dz, dy, dx, 1 - g.core), gco_sems.at[0, slot], gco_sems.at[1, slot]))

    def wait_for(src, dst, send_sem, recv_sem, device):
        copy = pltpu.make_async_remote_copy(
            src_ref=src, dst_ref=dst, send_sem=send_sem, recv_sem=recv_sem,
            device_id=device, device_id_type=pl.DeviceIdType.MESH,
        )
        copy.wait_recv()

    sent = []
    own = gathered.at[mine]
    for dz in range(1, n_hi):
        peer = g.at(step(g.hi, dz, n_hi), g.lo, g.x, g.core)
        sent.append(send(own, own, ghi_sems.at[0, dz], ghi_sems.at[1, dz], peer))
    loads[1].wait()
    acc[...] = jnp.zeros_like(acc)
    squares_ref[...] = jnp.zeros_like(squares_ref)

    def absorb(chunk):
        block = gathered[chunk].astype(F32)
        squares_ref[...] += jnp.sum(block * block, axis=1, keepdims=True)
        scaled = (block * gain_ref[chunk]).astype(BF16)
        acc[...] += jnp.dot(
            scaled, wup[pl.ds(pl.multiple_of(chunk * size, size), size), :],
            preferred_element_type=F32,
        )

    def take_sibling(item):
        place, other, chunk, send_sem, recv_sem = item
        copy = pltpu.make_async_remote_copy(
            src_ref=place, dst_ref=other, send_sem=send_sem, recv_sem=recv_sem,
            device_id=sibling, device_id_type=pl.DeviceIdType.MESH,
        )
        copy.wait_recv()
        copy.wait_send()
        absorb(chunk)

    for dz in range(n_hi):
        place = gathered.at[index(dz, 0, 0, g.core)]
        if dz:
            wait_for(own, place, ghi_sems.at[0, dz], ghi_sems.at[1, dz],
                     g.at(step(g.hi, dz, n_hi), g.lo, g.x, g.core))
        for p, d in enumerate(g.plane):
            sent.append(send(place, place, gpl_sems.at[0, dz, p], gpl_sems.at[1, dz, p],
                             plane_peers[d]))
        to_sibling(dz, 0, 0)
        absorb(index(dz, 0, 0, g.core))
    for dz in range(n_hi):
        for p, (dy, dx) in enumerate(g.plane):
            place = gathered.at[index(dz, dy, dx, g.core)]
            wait_for(own, place, gpl_sems.at[0, dz, p], gpl_sems.at[1, dz, p],
                     plane_peers[dy, dx])
            to_sibling(dz, dy, dx)
            absorb(index(dz, dy, dx, g.core))
            if pending:
                take_sibling(pending.pop(0))
    for item in pending:
        take_sibling(item)
    for copy in sent:
        copy.wait_send()

    n_dev = n_kv * n_tp
    scale = lax.rsqrt(squares_ref[...] / (n_dev * size) + EPSILON)
    hidden = jnp.square(jnp.maximum(acc[...] * scale, 0.0)).astype(BF16)
    loads[2].wait()
    width = n_tp * size

    def down(j):
        columns = pl.ds(pl.multiple_of(j * width, width), width)
        value = jnp.dot(hidden, wdown[:, columns], preferred_element_type=F32)
        for x in range(n_x):
            pair = [
                value[:, (x * g.n_core + c) * size : (x * g.n_core + c + 1) * size]
                for c in range(g.n_core)
            ]
            if g.n_core == 1:
                y_own[j, x] = pair[0]
            else:
                y_own[j, x] = jnp.where(g.core == 0, pair[0], pair[1])
                y_send[j, x] = jnp.where(g.core == 0, pair[1], pair[0]).astype(BF16)

    order = [(dz, dy) for dz in list(range(1, n_hi)) + [0] for dy in range(n_lo)]

    def kv_of(dz, dy):
        return step(g.hi, dz, n_hi) * n_lo + step(g.lo, dy, n_lo)

    swaps = {}
    for s, (dz, dy) in enumerate(order):
        j = kv_of(dz, dy)
        down(j)
        if sibling is not None:
            swaps[dz, dy] = send(y_send.at[j], y_recv.at[j], y_sems.at[0, s], y_sems.at[1, s],
                                 sibling)
    planes = {}
    for dz, dy in order:
        j = kv_of(dz, dy)
        if sibling is not None:
            swaps[dz, dy].wait()
        for dx in range(n_x):
            x = step(g.x, dx, n_x)
            total = y_own[j, x]
            if sibling is not None:
                total = total + y_recv[j, x].astype(F32)
            if (dy, dx) == (0, 0):
                last_total[dz] = total
            else:
                p = g.plane.index((dy, dx))
                p_send[dz, p] = total.astype(BF16)
                planes[dz, p] = send(p_send.at[dz, p], p_recv.at[dz, p], p_sems.at[0, dz, p],
                                     p_sems.at[1, dz, p], plane_peers[dy, dx])
    last = {}
    final = None
    for dz in list(range(1, n_hi)) + [0]:
        total = last_total[dz]
        for p in range(len(g.plane)):
            planes[dz, p].wait()
            total = total + p_recv[dz, p].astype(F32)
        if dz:
            f_send[dz] = total.astype(BF16)
            last[dz] = send(f_send.at[dz], f_recv.at[dz], f_sems.at[0, dz], f_sems.at[1, dz],
                           g.at(step(g.hi, dz, n_hi), g.lo, g.x, g.core))
        else:
            final = total
    for dz in range(1, n_hi):
        last[dz].wait()
        final = final + f_recv[dz].astype(F32)
    out_ref[...] = (gathered[mine].astype(F32) + final).astype(out_ref.dtype)


def layer(grid, tokens, mix_gain, weights, w_beta, w_decay, decay_rate, out_gain, state, w_out,
          mlp_gain, w_up, w_down):
    g = grid
    batch, size = tokens.shape
    n_dev = g.n_kv * g.n_tp
    rows, heads, head_size, _ = state.shape
    depth, width = weights[0].shape
    all_heads = w_beta.shape[1]
    lane_gap = -(-all_heads // 32) * 32
    lanes = -(-(2 * lane_gap + 1) // 128) * 128
    n_plane = max(1, len(g.plane))
    vmem = pl.BlockSpec(memory_space=pltpu.VMEM)
    hbm = pl.BlockSpec(memory_space=pltpu.HBM)
    dma = pltpu.SemaphoreType.DMA
    block = (batch, size)
    per_head = (heads, rows, head_size)
    buffers = [
        pltpu.VMEM((g.n_tp,) + block, BF16),
        pltpu.VMEM((4, depth, width), BF16),
        pltpu.VMEM((lanes, depth), BF16),
        pltpu.VMEM((4, g.n_kv, rows, width), F32),
        pltpu.VMEM((g.n_kv, rows, lanes), F32),
        pltpu.VMEM((g.n_kv, rows, lanes), F32),
        pltpu.VMEM((4, g.n_lo, g.n_hi, rows, width), BF16),
        pltpu.VMEM((4, g.n_lo, g.n_hi, rows, width), BF16),
        pltpu.VMEM((4, rows, width), F32),
        pltpu.VMEM((4, g.n_hi, rows, width), BF16),
        pltpu.VMEM((4, g.n_hi, rows, width), BF16),
        pltpu.VMEM(state.shape, F32),
        pltpu.VMEM(per_head, F32),
        pltpu.VMEM(per_head, F32),
        pltpu.VMEM(per_head, F32),
        pltpu.VMEM(per_head, F32),
        pltpu.VMEM((rows, width), F32),
        pltpu.VMEM((rows, width), F32),
        pltpu.VMEM(per_head, F32),
        pltpu.VMEM(per_head, F32),
        pltpu.VMEM(w_out.shape, BF16),
        pltpu.VMEM(w_up.shape, BF16),
        pltpu.VMEM(w_down.shape, BF16),
        pltpu.VMEM((g.n_kv, rows, width), BF16),
        pltpu.VMEM((g.n_tp,) + block, F32),
        pltpu.VMEM((g.n_tp,) + block, BF16),
        pltpu.VMEM((g.n_tp,) + block, BF16),
        pltpu.VMEM((n_dev,) + block, BF16),
        pltpu.VMEM((batch, w_up.shape[1]), F32),
        pltpu.VMEM((batch, 1), F32),
        pltpu.VMEM((g.n_kv, g.n_x) + block, F32),
        pltpu.VMEM((g.n_kv, g.n_x) + block, BF16),
        pltpu.VMEM((g.n_kv, g.n_x) + block, BF16),
        pltpu.VMEM((g.n_hi, n_plane) + block, BF16),
        pltpu.VMEM((g.n_hi, n_plane) + block, BF16),
        pltpu.VMEM((g.n_hi,) + block, F32),
        pltpu.VMEM((g.n_hi,) + block, BF16),
        pltpu.VMEM((g.n_hi,) + block, BF16),
    ]
    limit = VMEM_BYTES - SPARE_BYTES - padded_bytes(state.shape, F32)
    return pl.pallas_call(
        functools.partial(layer_kernel, g, all_heads, lane_gap, n_dev * size),
        out_shape=(
            jax.ShapeDtypeStruct(block, BF16),
            pltpu.VMEM(state.shape, F32),
        ),
        in_specs=[vmem] * 7 + [hbm] * 8,
        out_specs=(vmem,) * 2,
        scratch_shapes=buffers + [
            dma((4,)),
            dma((4,)),
            dma,
            dma((2, g.n_tp)),
            dma((2, g.n_kv)),
            dma((2, 4, g.n_lo)),
            dma((2, 4, g.n_hi)),
            dma((2, g.n_kv)),
            dma((2, g.n_tp)),
            dma((2, g.n_hi)),
            dma((2, g.n_hi, n_plane)),
            dma((2, g.n_kv * g.n_x)),
            dma((2, g.n_kv)),
            dma((2, g.n_hi, n_plane)),
            dma((2, g.n_hi)),
        ],
        compiler_params=pltpu.CompilerParams(
            collective_id=0, has_side_effects=True, vmem_limit_bytes=limit
        ),
        name="layer",
    )(
        tokens, mix_gain.reshape(g.n_tp, 1, size), w_beta.T, w_decay.T,
        decay_rate.reshape(1, heads), out_gain.reshape(1, head_size),
        mlp_gain.reshape(n_dev, 1, size), *weights, state, w_out, w_up, w_down,
    )


def local(
    n_kv, n_tp,
    tokens, mix_gain, w_query, w_key, w_value, w_gate, w_beta, w_decay, decay_rate, out_gain,
    state, w_out, mlp_gain, w_up, w_down,
):
    return layer(
        Grid(n_kv, n_tp), tokens, mix_gain, (w_key, w_query, w_value, w_gate), w_beta, w_decay,
        decay_rate, out_gain, state, w_out, mlp_gain, w_up, w_down,
    )


def solution(mesh):
    placed = (
        P(None, ("kv", "tp")),
        P("kv"),
        P("kv", "tp"),
        P("kv", "tp"),
        P("kv", "tp"),
        P("kv", "tp"),
        P("kv", None),
        P("kv", None),
        P("tp"),
        P(),
        P("kv", "tp", None, None),
        P("tp", "kv"),
        P(),
        P(None, ("kv", "tp")),
        P(("kv", "tp"), None),
    )
    return jax.shard_map(
        functools.partial(local, mesh.shape["kv"], mesh.shape["tp"]),
        mesh=mesh,
        in_specs=placed,
        out_specs=(P(None, ("kv", "tp")), P("kv", "tp", None, None)),
        check_vma=False,
    )
```
